128 devices in a mesh: rep: 2 (over z_hi), fs: 32 (over z_lo, y, x), tp: 2 (over core).
Axes of the slice: x: 4, y: 4, z: 4 (z_hi: 2, z_lo: 2; z = z_hi * 2 + z_lo), core: 2. Of those that a mesh axis runs over, the one named last changes fastest.
Arguments:
- residual: bfloat16 [32768, 2048], P(('rep', 'fs', 'tp')), may hold values from -6 to 6
- mixer_gain: float32 [2048], replicated, may hold values from 0.1 to 1.9
- gating_proj: bfloat16 [2048, 2048], P('fs', 'tp'), may hold values from -0.125 to 0.125
- spatial_proj: bfloat16 [2048, 2048], P('fs', 'tp'), as said below
- spatial_gain: float32 [2048], replicated, may hold values from 0.1 to 1.9
- spatial_bias: float32 [2048], replicated, may hold values from -3 to 3
- spatial_mix: bfloat16 [32, 128, 128], replicated, may hold values from -0.5 to 0.5
- spatial_offset: float32 [32, 128], replicated, may hold values from 0.5 to 1.5
- mixer_out: bfloat16 [2048, 2048], P('tp', 'fs'), may hold values from -0.125 to 0.125
- channel_gain: float32 [2048], replicated, may hold values from 0.1 to 1.9
- gate_proj: bfloat16 [2048, 2816], P('fs', 'tp'), may hold values from -0.125 to 0.125
- up_proj: bfloat16 [2048, 2816], P('fs', 'tp'), may hold values from -0.125 to 0.125
- conv_taps: float32 [3, 2816], replicated, may hold values from -3.5 to 3.5
- down_proj: bfloat16 [2816, 2048], P('tp', 'fs'), may hold values from -0.109375 to 0.109375
Outputs:
- layer_out: bfloat16 [32768, 2048], P(('rep', 'fs', 'tp'))
The draws below stay inside these ranges and needn't reach their ends.
Inputs may be any that keep to these rules, and one draw needn't show every extreme that they name: `spatial_proj`: entries are bounded in magnitude by 56 / sqrt(2048).
All inputs are finite; a program needn't handle non-finite values.
Results may differ from the reference program's by a relative error of at most 0.015.
Values may be sent and summed in bfloat16 or wider, within the bound.
No kernel may reach another device: no remote copies, remote signals or barrier semaphores. Data moves between devices by JAX's collectives and lax.ppermute only.
A program may use at most 128 MiB of HBM per device.

```python
import jax
import jax.numpy as jnp
from jax import lax

D = 2048
HEADS = 32
HEAD = 64
GROUP = 2048
BLOCK = 128
SEGMENT = 64
FF = 2816
KCONV = 3
SEQ_LEN = 256
TOKENS = 32768
N_TP = 2


def draw_spatial_proj(key, part):
    key_vals = jax.random.fold_in(key, 11)
    key_cols = jax.random.fold_in(key, 12)
    column = jnp.arange(GROUP).astype(jnp.float32)
    rising = jnp.power(10.0, column / (GROUP - 1))
    jitter = jax.random.uniform(key_cols, (GROUP,), jnp.float32, 0.7, 1.4)
    values = jnp.clip(jax.random.normal(key_vals, (D, GROUP), jnp.float32), -4.0, 4.0)
    return (values * rising * jitter * D ** (-0.5)).astype(jnp.bfloat16)


def level_of(own_key, dims, cuts, smallest, top_value):
    def one(dim, blocks):
        heights = jax.random.uniform(jax.random.fold_in(jax.random.fold_in(own_key, 6), dim), (blocks,), jnp.float32, smallest / len(cuts), top_value / len(cuts))
        return jnp.repeat(jnp.exp(heights), dims[dim] // blocks).reshape((-1,) + (1,) * (len(dims) - dim - 1))

    level = one(*cuts[0])
    for cut in cuts[1:]:
        level = level * one(*cut)
    return level


def bell_draw(own_key, dims, scale, reach, pieces=(), held_as=jnp.bfloat16):
    loudness = level_of(own_key, dims, pieces, -0.22, 0.18) if pieces else 1.0
    drawn = jax.random.normal(own_key, dims, jnp.float32) * scale * loudness
    return jnp.minimum(jnp.maximum(drawn, -reach), reach).astype(held_as)


def setup_inputs(seed: int = 0) -> dict:
    seeds = jax.random.split(jax.random.key(seed), 15)
    residual = bell_draw(seeds[0], (TOKENS, D), 1.0, 6.0, ((0, 128),))
    mixer_gain = jnp.clip(1.0 + 0.18 * jax.random.normal(seeds[1], (D,), jnp.float32), 0.1, 1.9)
    gating_proj = bell_draw(seeds[2], (D, GROUP), D ** -0.5, 0.125, ((0, 32), (1, 2)))
    spatial_proj = draw_spatial_proj(jax.random.fold_in(seeds[14], 71), 0)
    spatial_gain = jnp.clip(1.0 + 0.18 * jax.random.normal(seeds[4], (GROUP,), jnp.float32), 0.1, 1.9)
    spatial_bias = bell_draw(seeds[5], (GROUP,), 0.5, 3.0, (), jnp.float32)
    spatial_mix = bell_draw(seeds[6], (HEADS, BLOCK, BLOCK), BLOCK ** -0.5, 0.5)
    spatial_offset = jnp.clip(jax.random.uniform(seeds[7], (HEADS, BLOCK), jnp.float32, 0.5, 1.5), 0.5, 1.5)
    mixer_out = bell_draw(seeds[8], (GROUP, D), GROUP ** -0.5, 0.125, ((0, 2), (1, 32)))
    channel_gain = jnp.clip(1.0 + 0.18 * jax.random.normal(seeds[9], (D,), jnp.float32), 0.1, 1.9)
    gate_proj = bell_draw(seeds[10], (D, FF), D ** -0.5, 0.125, ((0, 32), (1, 2)))
    up_proj = bell_draw(seeds[11], (D, FF), D ** -0.5, 0.125, ((0, 32), (1, 2)))
    conv_taps = bell_draw(seeds[12], (KCONV, FF), KCONV ** -0.5, 3.5, (), jnp.float32)
    down_proj = bell_draw(seeds[13], (FF, D), FF ** -0.5, 0.109375, ((0, 2), (1, 32)))
    return dict(residual=residual, mixer_gain=mixer_gain, gating_proj=gating_proj, spatial_proj=spatial_proj, spatial_gain=spatial_gain, spatial_bias=spatial_bias, spatial_mix=spatial_mix, spatial_offset=spatial_offset, mixer_out=mixer_out, channel_gain=channel_gain, gate_proj=gate_proj, up_proj=up_proj, conv_taps=conv_taps, down_proj=down_proj)


def round_trip(value):
    return lax.optimization_barrier(value.astype(jnp.bfloat16)).astype(jnp.float32)

def rms_normed(value, gain):
    wide = value.astype(jnp.float32)
    scale = lax.rsqrt(lax.optimization_barrier(jnp.mean(wide * wide, axis=-1, keepdims=True)) + 1e-06)
    return (wide * scale * gain).astype(jnp.bfloat16)

def split_sum(left, right, parts):
    rows, inner = left.shape
    left_parts = left.reshape(rows, parts, inner // parts).astype(jnp.float32)
    right_parts = right.reshape(parts, inner // parts, right.shape[1]).astype(jnp.float32)
    terms = jnp.einsum('snc,ncd->nsd', left_parts, right_parts)
    return lax.optimization_barrier(jnp.sum(terms.astype(jnp.bfloat16).astype(jnp.float32), axis=0))

def one_sequence(args):
    rows, mixer_gain, gating_proj, spatial_proj, spatial_gain, spatial_bias, spatial_mix, spatial_offset, mixer_out, channel_gain, gate_proj, up_proj, conv_taps, down_proj = args
    normed = rms_normed(rows, mixer_gain)
    gating = round_trip(jnp.dot(normed, gating_proj, preferred_element_type=jnp.float32))
    spatial = round_trip(jnp.dot(normed, spatial_proj, preferred_element_type=jnp.float32))
    act_u = jax.nn.gelu(gating)
    act_v = jax.nn.gelu(spatial)
    mean = lax.optimization_barrier(jnp.sum(act_v, axis=-1, keepdims=True)) / GROUP
    var = lax.optimization_barrier(jnp.sum(act_v * act_v, axis=-1, keepdims=True)) / GROUP - mean * mean
    vnorm = ((act_v - mean) * lax.rsqrt(var + 1e-05) * spatial_gain + spatial_bias).astype(jnp.bfloat16)
    place = jnp.arange(BLOCK) // SEGMENT
    allowed = place[None, :] <= place[:, None]
    weights = jnp.where(allowed[None], spatial_mix, jnp.zeros_like(spatial_mix)).astype(jnp.float32)
    blocks = vnorm.reshape(SEQ_LEN // BLOCK, BLOCK, HEADS, HEAD).astype(jnp.float32)
    mixed = jnp.einsum('hij,njhd->nihd', weights, blocks) + spatial_offset.T[None, :, :, None]
    gated = (act_u * mixed.reshape(SEQ_LEN, GROUP)).astype(jnp.bfloat16)
    middle = (rows.astype(jnp.float32) + split_sum(gated, mixer_out, N_TP)).astype(jnp.bfloat16)
    normed2 = rms_normed(middle, channel_gain)
    gate = round_trip(jnp.dot(normed2, gate_proj, preferred_element_type=jnp.float32))
    up = round_trip(jnp.dot(normed2, up_proj, preferred_element_type=jnp.float32))
    padded = jnp.concatenate([jnp.zeros((KCONV - 1, FF), jnp.float32), gate], axis=0)
    conv = jnp.zeros((SEQ_LEN, FF), jnp.float32)
    for tap in range(KCONV):
        conv = conv + conv_taps[tap] * padded[tap:tap + SEQ_LEN]
    hidden = (jax.nn.silu(conv) * up).astype(jnp.bfloat16)
    return (middle.astype(jnp.float32) + split_sum(hidden, down_proj, N_TP)).astype(jnp.bfloat16)

def reference(residual, mixer_gain, gating_proj, spatial_proj, spatial_gain, spatial_bias, spatial_mix, spatial_offset, mixer_out, channel_gain, gate_proj, up_proj, conv_taps, down_proj):
    shaped = residual.reshape(residual.shape[0] // SEQ_LEN, SEQ_LEN, D)

    def apply(rows):
        return one_sequence((rows, mixer_gain, gating_proj, spatial_proj, spatial_gain, spatial_bias, spatial_mix, spatial_offset, mixer_out, channel_gain, gate_proj, up_proj, conv_taps, down_proj))
    result = lax.map(apply, shaped)
    return result.reshape(residual.shape[0], D)
```

```python
import functools

import jax
import jax.numpy as jnp
from jax import lax
from jax.experimental import pallas as pl
from jax.experimental.pallas import tpu as pltpu
from jax.sharding import Mesh
from jax.sharding import PartitionSpec as P

D = 2048
HEAD = 64
GROUP = 2048
BLOCK = 128
SEGMENT = 64
SEQ = 256
QM = 512
QC = 768
QSTEP = 640
UNITS = 1408
FS = ("fs_0", "fs_1", "fs_2")
REP_FS_TP = ("rep", "fs_0", "fs_1", "fs_2", "tp")
Z = ("rep", "fs_0")
ZT = ("rep", "fs_0", "tp")
X = "fs_2"
Y = "fs_1"
F32 = jnp.float32
BF16 = jnp.bfloat16


def ring(value, axis, by):
    return lax.ppermute(value, axis, [(i, (i + by) % 4) for i in range(4)])


def other_core(value):
    return lax.ppermute(value, "tp", [(0, 1), (1, 0)])


def to_partner(value):
    pairs = []
    for z in range(4):
        pairs.append((2 * z, 2 * ((z - 1) % 4)))
        pairs.append((2 * z + 1, 2 * ((z + 1) % 4) + 1))
    return lax.ppermute(value, ZT, pairs)


def to_owner(value):
    pairs = []
    for z in range(4):
        pairs.append((2 * z, 2 * ((z + 1) % 4)))
        pairs.append((2 * z + 1, 2 * ((z - 1) % 4) + 1))
    return lax.ppermute(value, ZT, pairs)


def plane_first(piece, first):
    back = ring(piece, first, 1)
    ahead = ring(piece, first, -1)
    far = ring(piece, first, 2)
    return jnp.concatenate([piece, ahead, far, back], axis=0)


def plane_second(line, second):
    back = ring(line, second, 1)
    ahead = ring(line, second, -1)
    far_top = ring(back[:128], second, 1)
    far_bottom = ring(ahead[128:], second, -1)
    return (line, ahead, far_top, far_bottom, back)


PLACES = []
for _f in range(4):
    for _s in range(4):
        if _s == 0:
            PLACES.append((0, _f * 64, _f, _s))
        elif _s == 1:
            PLACES.append((1, _f * 64, _f, _s))
        elif _s == 3:
            PLACES.append((4, _f * 64, _f, _s))
        elif _f < 2:
            PLACES.append((2, _f * 64, _f, _s))
        else:
            PLACES.append((3, (_f - 2) * 64, _f, _s))


def weight_copies(refs, held, sems, column, width, base):
    x = lax.axis_index("fs_2")
    y = lax.axis_index("fs_1")
    a = lax.axis_index("fs_0")
    copies = []
    for stream in range(2):
        for k, (which, row, first, second) in enumerate(PLACES):
            dx, dy = (first, second) if stream == 0 else (second, first)
            block = lax.rem(a + stream, 2) * 16 + lax.rem(y + dy, 4) * 4 + lax.rem(x + dx, 4)
            to = pl.multiple_of(block * 64, 64)
            copies.append(
                pltpu.make_async_copy(
                    refs[stream * 5 + which].at[pl.ds(row, 64), pl.ds(column, width)],
                    held.at[pl.ds(to, 64), :],
                    sems.at[base + stream * 16 + k],
                )
            )
    return copies


def rms_normed(value, gain):
    wide = value.astype(F32)
    scale = lax.rsqrt(jnp.mean(wide * wide, axis=-1, keepdims=True) + 1e-06)
    return (wide * scale * gain).astype(BF16)


def as_row(column):
    return jnp.broadcast_to(column, (BLOCK, BLOCK)).T[0:1, :]


def as_column(row):
    return jnp.broadcast_to(row, (BLOCK, BLOCK)).T


def spatial_kernel(own, own2, rem, rem2, gain, *rest):
    pieces, (normed, act_v, sums), (held, sems) = rest[:10], rest[10:13], rest[13:]
    t = lax.axis_index("tp")
    copies = weight_copies(pieces, held, sems, 0, QM, 0)
    for c in copies:
        c.start()
    for s, ref in enumerate((own, own2, rem, rem2)):

        @pl.loop(0, SEQ // 64)
        def _(k):
            rows = pl.ds(pl.multiple_of(k * 64, 64), 64)
            normed[pl.ds(pl.multiple_of(s * SEQ + k * 64, 64), 64), :] = rms_normed(ref[rows, :], gain[...])

    for c in copies:
        c.wait()

    @pl.loop(0, 4)
    def _(s):
        rows = pl.ds(pl.multiple_of(s * SEQ, SEQ), SEQ)
        v = jnp.dot(normed[rows, :], held[...], preferred_element_type=F32)
        v = jax.nn.gelu(v.astype(BF16).astype(F32))
        act_v[rows, :] = v
        place = 2 * (s // 2) + lax.rem(lax.rem(s, 2) + t, 2)
        total = jnp.sum(v, axis=-1, keepdims=True)
        squares = jnp.sum(v * v, axis=-1, keepdims=True)
        for b in range(2):
            part = slice(b * BLOCK, (b + 1) * BLOCK)
            sums[place, b : b + 1, :] = as_row(total[part])
            sums[place, 2 + b : 3 + b, :] = as_row(squares[part])


def gating_kernel(normed, *rest):
    pieces, (act_u,), (held, sems) = rest[:10], rest[10:11], rest[11:]
    copies = weight_copies(pieces, held, sems, QM, QM, 0)
    for c in copies:
        c.start()
    for c in copies:
        c.wait()

    @pl.loop(0, 4)
    def _(s):
        rows = pl.ds(pl.multiple_of(s * SEQ, SEQ), SEQ)
        u = jnp.dot(normed[rows, :], held[...], preferred_element_type=F32)
        act_u[rows, :] = jax.nn.gelu(u.astype(BF16).astype(F32))


def mix_kernel(act_u, act_v, sums, gain, bias, mix, offset, *rest):
    pieces, outs, (held, gated, sems) = rest[:10], rest[10:14], rest[14:]
    t = lax.axis_index("tp")
    copies = weight_copies(pieces, held, sems, 2 * QM, QM, 0)
    for c in copies:
        c.start()

    @pl.loop(0, 4)
    def _(s):
        place = 2 * (s // 2) + lax.rem(lax.rem(s, 2) + t, 2)
        for b in range(2):
            rows = pl.ds(pl.multiple_of(s * SEQ + b * BLOCK, BLOCK), BLOCK)
            mean = as_column(sums[place, b : b + 1, :]) / GROUP
            var = as_column(sums[place, 2 + b : 3 + b, :]) / GROUP - mean * mean
            scale = lax.rsqrt(var + 1e-05)
            for c in range(QM // 128):
                lanes = slice(c * 128, (c + 1) * 128)
                v = (act_v[rows, lanes] - mean) * scale * gain[:, lanes] + bias[:, lanes]
                both = jnp.dot(mix[c], v.astype(BF16), preferred_element_type=F32)
                lane = lax.broadcasted_iota(jnp.int32, (BLOCK, 128), 1)
                mixed = jnp.where(lane < HEAD, both[:BLOCK], both[BLOCK:]) + offset[:, lanes]
                gated[rows, lanes] = (act_u[rows, lanes] * mixed).astype(BF16)

    for c in copies:
        c.wait()
    for s in range(4):
        out = lax.dot_general(
            gated[s * SEQ : (s + 1) * SEQ, :], held[...], (((1,), (1,)), ((), ())), preferred_element_type=F32
        )
        outs[s][...] = out.astype(BF16)


def channel_kernel(own, own2, rem, rem2, gain, taps, *rest):
    pieces, outs, (normed, wgate, wup, wdown, sems) = rest[:10], rest[10:14], rest[14:]
    a = lax.axis_index("fs_0")
    copies = weight_copies(pieces, wgate, sems, 0, QC, 0)
    copies += weight_copies(pieces, wup, sems, QC, QC, 32)
    copies += weight_copies(pieces, wdown, sems, 2 * QC, QC, 64)
    for c in copies:
        c.start()
    for s, ref in enumerate((own, own2, rem, rem2)):

        @pl.loop(0, SEQ // 64)
        def _(k):
            rows = pl.ds(pl.multiple_of(k * 64, 64), 64)
            normed[pl.ds(pl.multiple_of(s * SEQ + k * 64, 64), 64), :] = rms_normed(ref[rows, :], gain[...])

    for c in copies:
        c.wait()
    for s in range(4):
        n = normed[s * SEQ : (s + 1) * SEQ, :]
        gate = jnp.dot(n, wgate[...], preferred_element_type=F32).astype(BF16).astype(F32)
        up = jnp.dot(n, wup[...], preferred_element_type=F32).astype(BF16).astype(F32)
        row = lax.broadcasted_iota(jnp.int32, gate.shape, 0)
        conv = taps[2:3, :] * gate
        for lag in (1, 2):
            conv = conv + taps[2 - lag : 3 - lag, :] * jnp.where(row >= lag, pltpu.roll(gate, lag, 0), 0.0)
        hidden = jax.nn.silu(conv) * up
        lane = lax.broadcasted_iota(jnp.int32, gate.shape, 1)
        hidden = jnp.where(lane >= 128 * a, hidden, 0.0).astype(BF16)
        out = lax.dot_general(hidden, wdown[...], (((1,), (1,)), ((), ())), preferred_element_type=F32)
        outs[s][...] = out.astype(BF16)


VM = pl.BlockSpec(memory_space=pltpu.VMEM)
AN = pl.BlockSpec(memory_space=pl.ANY)


def call(kernel, name, n_in, out_shape, scratch, flops, args):
    return pl.pallas_call(
        kernel,
        out_shape=out_shape,
        in_specs=[VM] * n_in + [AN] * 10,
        out_specs=jax.tree.map(lambda _: VM, out_shape),
        scratch_shapes=scratch,
        name=name,
        cost_estimate=pl.CostEstimate(flops=int(flops), bytes_accessed=8 << 20, transcendentals=0),
        compiler_params=pltpu.CompilerParams(vmem_limit_bytes=60 << 20),
    )(*args)


def arr(shape, dtype):
    return jax.ShapeDtypeStruct(shape, dtype)


def on_device(
    residual,
    mixer_gain,
    gating_proj,
    spatial_proj,
    spatial_gain,
    spatial_bias,
    spatial_mix,
    spatial_offset,
    mixer_out,
    channel_gain,
    gate_proj,
    up_proj,
    conv_taps,
    down_proj,
):
    a = lax.axis_index("fs_0")
    t = lax.axis_index("tp")

    def window(arrays, which, step, width):
        return jnp.concatenate(
            [lax.dynamic_slice_in_dim(w, which * step, width, 1) for w in arrays], axis=1
        )

    mixer_arrays = (spatial_proj, gating_proj, mixer_out.T)
    channel_arrays = (gate_proj, up_proj, down_proj.T)
    m_own = window(mixer_arrays, a, QM, QM)
    m_give = window(mixer_arrays, 1 - a, QM, QM)
    c_own = window(channel_arrays, a, QSTEP, QC)
    c_give = window(channel_arrays, 1 - a, QSTEP, QC)

    def z_swap(give):
        return jnp.concatenate([ring(give[:32], Z, 1), ring(give[32:], Z, -1)], axis=0)

    own = residual
    own2 = other_core(own)
    m_a = plane_first(m_own, X)
    m_b = plane_first(z_swap(m_give), Y)
    rem = to_partner(own)
    rem2 = other_core(rem)
    m_pieces = plane_second(m_a, Y) + plane_second(m_b, X)
    c_a = plane_first(c_own, X)
    c_b = plane_first(z_swap(c_give), Y)
    c_pieces = plane_second(c_a, Y) + plane_second(c_b, X)

    normed, act_v, sums = call(
        spatial_kernel,
        "spatial",
        5,
        (arr((4 * SEQ, D), BF16), arr((4 * SEQ, QM), F32), arr((4, 4, 128), F32)),
        [pltpu.VMEM((D, QM), BF16), pltpu.SemaphoreType.DMA((32,))],
        2 * 1024 * D * QM,
        (own, own2, rem, rem2, mixer_gain[None], *m_pieces),
    )
    sums = sums + other_core(sums)
    from_below = ring(sums[1:3], Z, 1)
    from_above = ring(jnp.stack([sums[0], sums[3]]), Z, -1)
    sums = sums + jnp.stack([from_below[1], from_above[1], from_above[0], from_below[0]])
    (act_u,) = call(
        gating_kernel,
        "gating",
        1,
        (arr((4 * SEQ, QM), F32),),
        [pltpu.VMEM((D, QM), BF16), pltpu.SemaphoreType.DMA((32,))],
        2 * 1024 * D * QM,
        (normed, *m_pieces),
    )
    start = t * 1024 + a * QM
    gain_here = lax.dynamic_slice_in_dim(spatial_gain, start, QM)[None]
    bias_here = lax.dynamic_slice_in_dim(spatial_bias, start, QM)[None]
    mix_here = lax.dynamic_slice_in_dim(spatial_mix, t * 16 + a * 8, 8, 0)
    offset_here = lax.dynamic_slice_in_dim(spatial_offset, t * 16 + a * 8, 8, 0)
    place = jnp.arange(BLOCK) // SEGMENT
    allowed = place[None, :] <= place[:, None]
    mix_here = jnp.where(allowed[None], mix_here, jnp.zeros_like(mix_here)).reshape(4, 256, 128)
    offset_here = jnp.repeat(offset_here.T, HEAD, axis=1)
    seqs = (arr((SEQ, D), BF16),) * 4
    parts = call(
        mix_kernel,
        "mix",
        7,
        seqs,
        [pltpu.VMEM((D, QM), BF16), pltpu.VMEM((4 * SEQ, QM), BF16), pltpu.SemaphoreType.DMA((32,))],
        2 * 1024 * D * QM,
        (act_u, act_v, sums, gain_here, bias_here, mix_here, offset_here, *m_pieces),
    )

    def plus(*arrays):
        total = arrays[0].astype(F32)
        for other in arrays[1:]:
            total = total + other.astype(F32)
        return total.astype(BF16)

    s_own = plus(parts[0], other_core(parts[1]))
    s_rem = plus(parts[2], other_core(parts[3]))
    mid_own = plus(own, s_own, to_owner(s_rem))
    mid_rem = plus(rem, s_rem, to_partner(s_own))
    mid_own2 = other_core(mid_own)
    mid_rem2 = other_core(mid_rem)
    taps_here = lax.dynamic_slice_in_dim(conv_taps, t * UNITS + a * QSTEP, QC, 1)
    parts = call(
        channel_kernel,
        "channel",
        6,
        seqs,
        [pltpu.VMEM((4 * SEQ, D), BF16)]
        + [pltpu.VMEM((D, QC), BF16)] * 3
        + [pltpu.SemaphoreType.DMA((96,))],
        6 * 1024 * D * QC,
        (mid_own, mid_own2, mid_rem, mid_rem2, channel_gain[None], taps_here, *c_pieces),
    )
    s_own = plus(parts[0], other_core(parts[1]))
    s_rem = plus(parts[2], other_core(parts[3]))
    return plus(mid_own, s_own, to_owner(s_rem))


def solution(mesh):
    split = Mesh(
        mesh.devices.reshape(mesh.shape["rep"], 2, 4, 4, mesh.shape["tp"]),
        ("rep", "fs_0", "fs_1", "fs_2", "tp"),
    )
    placed = (
        P(REP_FS_TP, None),
        P(),
        P(FS, "tp"),
        P(FS, "tp"),
        P(),
        P(),
        P(),
        P(),
        P("tp", FS),
        P(),
        P(FS, "tp"),
        P(FS, "tp"),
        P(),
        P("tp", FS),
    )
    return jax.shard_map(
        on_device, mesh=split, in_specs=placed, out_specs=P(REP_FS_TP, None), check_vma=False
    )
```

```python
import functools

import jax
import jax.numpy as jnp
from jax import lax
from jax.experimental import pallas as pl
from jax.experimental.pallas import tpu as pltpu
from jax.sharding import Mesh
from jax.sharding import PartitionSpec as P


D = 2048
HEAD = 64
GROUP = 2048
BLOCK = 128
SEGMENT = 64
SEQ = 256
QM = 512
QC = 768
QSTEP = 640
UNITS = 1408
FS = ("fs_0", "fs_1", "fs_2")
REP_FS_TP = ("rep", "fs_0", "fs_1", "fs_2", "tp")
Z = ("rep", "fs_0")
ZT = ("rep", "fs_0", "tp")
YXT = ("fs_1", "fs_2", "tp")
F32 = jnp.float32
BF16 = jnp.bfloat16


def ring(value, axis, by):
    return lax.ppermute(value, axis, [(i, (i + by) % 4) for i in range(4)])


def other_core(value):
    return lax.ppermute(value, "tp", [(0, 1), (1, 0)])


def to_partner(value):
    pairs = []
    for z in range(4):
        pairs.append((2 * z, 2 * ((z - 1) % 4)))
        pairs.append((2 * z + 1, 2 * ((z + 1) % 4) + 1))
    return lax.ppermute(value, ZT, pairs)


def to_owner(value):
    pairs = []
    for z in range(4):
        pairs.append((2 * z, 2 * ((z + 1) % 4)))
        pairs.append((2 * z + 1, 2 * ((z - 1) % 4) + 1))
    return lax.ppermute(value, ZT, pairs)


def along(value, first, by):
    pairs = []
    for y in range(4):
        for x in range(4):
            for t in range(2):
                on_x = (t == 0) == first
                to_x = (x + by) % 4 if on_x else x
                to_y = y if on_x else (y + by) % 4
                pairs.append((y * 8 + x * 2 + t, to_y * 8 + to_x * 2 + t))
    return lax.ppermute(value, YXT, pairs)


def plane_first(piece, route):
    back = along(piece, True, 1)
    ahead = along(piece, True, -1)
    return (piece, ahead, furthest(piece, ahead, back, True, route), back)


def furthest(piece, ahead, back, first, route):
    if route == 0:
        return along(piece, first, 2)
    return along(back, first, 1) if route > 0 else along(ahead, first, -1)


def join_kernel(widths, *refs):
    pieces, outs, sems = refs[:8], refs[8:-1], refs[-1]
    copies = []
    column = 0
    for k, width in enumerate(widths):
        for n, piece in enumerate(pieces):
            copies.append(
                pltpu.make_async_copy(
                    piece.at[:, pl.ds(column, width)], outs[k].at[pl.ds(n * 64, 64), :], sems.at[k * 8 + n]
                )
            )
        column += width
    for c in copies:
        c.start()
    for c in copies:
        c.wait()


def joined(pieces, widths):
    return pl.pallas_call(
        functools.partial(join_kernel, widths),
        out_shape=[jax.ShapeDtypeStruct((512, w), BF16) for w in widths],
        in_specs=[AN] * 8,
        out_specs=[VM] * len(widths),
        scratch_shapes=[pltpu.SemaphoreType.DMA((8 * len(widths),))],
        cost_estimate=pl.CostEstimate(flops=1 << 20, bytes_accessed=4 << 20, transcendentals=0),
        compiler_params=pltpu.CompilerParams(vmem_limit_bytes=6 << 20),
    )(*pieces)


def plane_second(line, route):
    back = along(line, False, 1)
    ahead = along(line, False, -1)
    return (line, ahead, furthest(line, ahead, back, False, route), back)


PLACES = [(s, f * 128 + h * 64, f, s, h) for s in range(4) for f in range(4) for h in range(2)]


def place_weight(refs, held):
    x = lax.axis_index("fs_2")
    y = lax.axis_index("fs_1")
    a = lax.axis_index("fs_0")
    t = lax.axis_index("tp")
    for which, row, first, second, half in PLACES:
        dx = first + t * (second - first)
        dy = second + t * (first - second)
        block = lax.rem(a + half, 2) * 16 + lax.rem(y + dy, 4) * 4 + lax.rem(x + dx, 4)
        held[pl.ds(pl.multiple_of(block * 64, 64), 64), :] = refs[which][row : row + 64, :]


def rms_normed(value, gain):
    wide = value.astype(F32)
    scale = lax.rsqrt(jnp.mean(wide * wide, axis=-1, keepdims=True) + 1e-06)
    return (wide * scale * gain).astype(BF16)


def norm_kernel(rows_in, gain, out):
    @pl.loop(0, SEQ // 32)
    def _(k):
        rows = pl.ds(pl.multiple_of(k * 32, 32), 32)
        out[rows, :] = rms_normed(rows_in[rows, :], gain[...])


def as_row(column):
    return jnp.broadcast_to(column, (BLOCK, BLOCK)).T[0:1, :]


def as_column(row):
    return jnp.broadcast_to(row, (BLOCK, BLOCK)).T


def spatial_kernel(own, own2, rem, rem2, *rest):
    pieces, (act_v, sums), (held,) = rest[:4], rest[4:6], rest[6:]
    t = lax.axis_index("tp")
    place_weight(pieces, held)
    for s, ref in enumerate((own, own2, rem, rem2)):
        v = jnp.dot(ref[...], held[...], preferred_element_type=F32)
        v = jax.nn.gelu(v.astype(BF16).astype(F32))
        act_v[s * SEQ : (s + 1) * SEQ, :] = v
        place = 2 * (s // 2) + lax.rem(s + t, 2)
        total = jnp.sum(v, axis=-1, keepdims=True)
        squares = jnp.sum(v * v, axis=-1, keepdims=True)
        for b in range(2):
            part = slice(b * BLOCK, (b + 1) * BLOCK)
            sums[place, b : b + 1, :] = as_row(total[part])
            sums[place, 2 + b : 3 + b, :] = as_row(squares[part])


def gating_kernel(own, own2, rem, rem2, *rest):
    pieces, (act_u,), (held,) = rest[:4], rest[4:5], rest[5:]
    place_weight(pieces, held)
    for s, ref in enumerate((own, own2, rem, rem2)):
        u = jnp.dot(ref[...], held[...], preferred_element_type=F32)
        act_u[s * SEQ : (s + 1) * SEQ, :] = jax.nn.gelu(u.astype(BF16).astype(F32))


def mix_kernel(pair, act_u, act_v, sums, gain, bias, offset, mix_all, *rest):
    pieces, outs, (held, gated, mix, shift) = rest[:4], rest[4:6], rest[6:]
    t = lax.axis_index("tp")
    a = lax.axis_index("fs_0")
    place_weight(pieces, held)
    start = pl.multiple_of(t * 1024 + a * QM, QM)
    gains = gain[:, pl.ds(start, QM)]
    biases = bias[:, pl.ds(start, QM)]
    lane = lax.broadcasted_iota(jnp.int32, (BLOCK, 128), 1)
    first_head = pl.multiple_of(t * 16 + a * 8, 8)
    offsets = offset[pl.ds(first_head, 8), :]
    for c in range(QM // 128):
        one, two = as_column(offsets[2 * c : 2 * c + 1]), as_column(offsets[2 * c + 1 : 2 * c + 2])
        shift[:, c * 128 : (c + 1) * 128] = jnp.where(lane < HEAD, one, two)
    allowed = lane // SEGMENT <= lax.broadcasted_iota(jnp.int32, (BLOCK, BLOCK), 0) // SEGMENT
    for h in range(8):
        mix[h] = jnp.where(allowed, mix_all[first_head + h].astype(F32), 0.0).astype(BF16)

    @pl.loop(0, 2)
    def _(s):
        place = 2 * pair + lax.rem(s + t, 2)
        for b in range(2):
            here = s * SEQ + b * BLOCK
            rows = pl.ds(pl.multiple_of(2 * pair * SEQ + here, BLOCK), BLOCK)
            to = pl.ds(pl.multiple_of(here, BLOCK), BLOCK)
            mean = as_column(sums[place, b : b + 1, :]) / GROUP
            var = as_column(sums[place, 2 + b : 3 + b, :]) / GROUP - mean * mean
            scale = lax.rsqrt(var + 1e-05)
            for c in range(QM // 128):
                lanes = slice(c * 128, (c + 1) * 128)
                v = (act_v[rows, lanes] - mean) * scale * gains[:, lanes] + biases[:, lanes]
                v = v.astype(BF16)
                one = jnp.dot(mix[2 * c], v, preferred_element_type=F32)
                two = jnp.dot(mix[2 * c + 1], v, preferred_element_type=F32)
                mixed = jnp.where(lane < HEAD, one, two) + shift[:, lanes]
                gated[to, lanes] = (act_u[rows, lanes] * mixed).astype(BF16)

    for s in (1, 0):
        out = lax.dot_general(
            gated[s * SEQ : (s + 1) * SEQ, :], held[...], (((1,), (1,)), ((), ())), preferred_element_type=F32
        )
        outs[s][...] = out.astype(BF16)


def assemble_kernel(*refs):
    n = len(refs) // 5
    for k in range(n):
        place_weight(refs[4 * k : 4 * k + 4], refs[4 * n + k])


def hidden_kernel(first, second, wgate, wup, taps_all, hidden):
    a = lax.axis_index("fs_0")
    t = lax.axis_index("tp")
    taps = taps_all[:, pl.ds(pl.multiple_of(t * UNITS + a * QSTEP, 128), QC)]
    for s, ref in enumerate((first, second)):
        gate = jnp.dot(ref[...], wgate[...], preferred_element_type=F32).astype(BF16).astype(F32)
        up = jnp.dot(ref[...], wup[...], preferred_element_type=F32).astype(BF16).astype(F32)
        row = lax.broadcasted_iota(jnp.int32, gate.shape, 0)
        conv = taps[2:3, :] * gate
        for lag in (1, 2):
            conv = conv + taps[2 - lag : 3 - lag, :] * jnp.where(row >= lag, pltpu.roll(gate, lag, 0), 0.0)
        product = jax.nn.silu(conv) * up
        lane = lax.broadcasted_iota(jnp.int32, gate.shape, 1)
        hidden[s] = jnp.where(lane >= 128 * a, product, 0.0).astype(BF16)


def down_kernel(hidden, wdown, out_first, out_second):
    for s, out_ref in ((1, out_second), (0, out_first)):
        out = lax.dot_general(hidden[s], wdown[...], (((1,), (1,)), ((), ())), preferred_element_type=F32)
        out_ref[...] = out.astype(BF16)


VM = pl.BlockSpec(memory_space=pltpu.VMEM)
AN = pl.BlockSpec(memory_space=pltpu.HBM)


def call(kernel, out_shape, scratch, flops, limit, args):
    return pl.pallas_call(
        kernel,
        out_shape=out_shape,
        in_specs=[VM] * len(args),
        out_specs=jax.tree.map(lambda _: VM, out_shape),
        scratch_shapes=scratch,
        cost_estimate=pl.CostEstimate(flops=int(flops), bytes_accessed=8 << 20, transcendentals=0),
        compiler_params=pltpu.CompilerParams(vmem_limit_bytes=limit << 20),
    )(*args)


def plus_kernel(n, gained, *refs):
    @pl.loop(0, SEQ // 32)
    def _(k):
        rows = pl.ds(pl.multiple_of(k * 32, 32), 32)
        total = refs[0][rows, :].astype(F32)
        for ref in refs[1:n]:
            total = total + ref[rows, :].astype(F32)
        total = total.astype(BF16)
        if gained:
            refs[n + 1][rows, :] = total
            refs[n + 2][rows, :] = rms_normed(total, refs[n][...])
        else:
            refs[n][rows, :] = total


def plus(*arrays, gain=None):
    one = jax.ShapeDtypeStruct((SEQ, D), BF16)
    args = arrays if gain is None else (*arrays, gain)
    return pl.pallas_call(
        functools.partial(plus_kernel, len(arrays), gain is not None),
        out_shape=one if gain is None else (one, one),
        in_specs=[VM] * len(args),
        out_specs=VM if gain is None else (VM, VM),
        cost_estimate=pl.CostEstimate(flops=1 << 20, bytes_accessed=4 << 20, transcendentals=0),
        compiler_params=pltpu.CompilerParams(vmem_limit_bytes=10 << 20),
    )(*args)


def normed(rows, gain):
    return pl.pallas_call(
        norm_kernel,
        out_shape=jax.ShapeDtypeStruct((SEQ, D), BF16),
        in_specs=[VM, VM],
        out_specs=VM,
        cost_estimate=pl.CostEstimate(flops=1 << 20, bytes_accessed=2 << 20, transcendentals=0),
        compiler_params=pltpu.CompilerParams(vmem_limit_bytes=6 << 20),
    )(rows, gain)


def arr(shape, dtype):
    return jax.ShapeDtypeStruct(shape, dtype)


def on_device(
    residual,
    mixer_gain,
    gating_proj,
    spatial_proj,
    spatial_gain,
    spatial_bias,
    spatial_mix,
    spatial_offset,
    mixer_out,
    channel_gain,
    gate_proj,
    up_proj,
    conv_taps,
    down_proj,
):
    a = lax.axis_index("fs_0")

    def window(arrays, which, step, width):
        return jnp.concatenate(
            [lax.dynamic_slice_in_dim(w, which * step, width, 1) for w in arrays], axis=1
        )

    mixer_arrays = (spatial_proj, gating_proj, mixer_out.T)
    channel_arrays = (gate_proj, up_proj, down_proj.T)

    def first_phase(arrays, step, width, by, routes):
        give = window(arrays, 1 - a, step, width)
        mine = window(arrays, a, step, width)
        theirs = ring(give, Z, by)
        firsts = zip(plane_first(mine, routes[0]), plane_first(theirs, routes[1]))
        return [piece for both in firsts for piece in both]

    own = residual
    rem = to_partner(own)
    own_n = normed(own, mixer_gain[None])
    own2_n = other_core(own_n)
    rem_n = normed(rem, mixer_gain[None])
    rem2_n = other_core(rem_n)
    m_first = first_phase(mixer_arrays, QM, QM, 1, (0, 0))
    s_line, u_line, o_line = joined(m_first, (QM,) * 3)
    s_pieces = plane_second(s_line, 1)
    u_pieces = plane_second(u_line, -1)
    o_pieces = plane_second(o_line, 0)
    c_first = first_phase(channel_arrays, QSTEP, QC, -1, (1, -1))
    g_line, h_line, d_line = joined(c_first, (QC,) * 3)
    g_pieces = plane_second(g_line, 1)
    h_pieces = plane_second(h_line, -1)
    d_pieces = plane_second(d_line, 0)
    seqs = (own_n, own2_n, rem_n, rem2_n)

    act_v, sums = call(
        spatial_kernel,
        (arr((4 * SEQ, QM), F32), arr((4, 4, 128), F32)),
        [pltpu.VMEM((D, QM), BF16)],
        2 * 1024 * D * QM,
        14,
        (*seqs, *s_pieces),
    )
    sums = sums + other_core(sums)
    from_below = ring(sums[1:3], Z, 1)
    from_above = ring(jnp.stack([sums[0], sums[3]]), Z, -1)
    sums = sums + jnp.stack([from_below[1], from_above[1], from_above[0], from_below[0]])
    (act_u,) = call(
        gating_kernel,
        (arr((4 * SEQ, QM), F32),),
        [pltpu.VMEM((D, QM), BF16)],
        2 * 1024 * D * QM,
        14,
        (*seqs, *u_pieces),
    )
    pair = (arr((SEQ, D), BF16),) * 2

    def mixed(k):
        return call(
            functools.partial(mix_kernel, k),
            pair,
            [pltpu.VMEM((D, QM), BF16), pltpu.VMEM((2 * SEQ, QM), BF16), pltpu.VMEM((8, 128, 128), BF16)]
            + [pltpu.VMEM((128, QM), F32)],
            1024 * D * QM,
            16,
            (act_u, act_v, sums, spatial_gain[None], spatial_bias[None], spatial_offset, spatial_mix, *o_pieces),
        )

    part, part2 = mixed(0)
    s_own = plus(part, other_core(part2))
    part, part2 = mixed(1)
    s_rem = plus(part, other_core(part2))
    _, rem_n = plus(rem, s_rem, to_partner(s_own), gain=channel_gain[None])
    mid_own, own_n = plus(own, s_own, to_owner(s_rem), gain=channel_gain[None])
    rem2_n = other_core(rem_n)
    own2_n = other_core(own_n)

    def assembled(*groups):
        flat = [p for g in groups for p in g]
        return pl.pallas_call(
            assemble_kernel,
            out_shape=[arr((D, QC), BF16)] * len(groups),
            in_specs=[VM] * len(flat),
            out_specs=[VM] * len(groups),
            cost_estimate=pl.CostEstimate(flops=1 << 20, bytes_accessed=8 << 20, transcendentals=0),
            compiler_params=pltpu.CompilerParams(vmem_limit_bytes=16 << 20),
        )(*flat)

    wgate, wup = assembled(g_pieces, h_pieces)
    (wdown,) = assembled(d_pieces)

    def hid(first, second):
        (out,) = call(
            hidden_kernel, (arr((2, SEQ, QC), BF16),), [], 2 * 1024 * D * QC, 20, (first, second, wgate, wup, conv_taps)
        )
        return out

    def down(hidden):
        return call(down_kernel, pair, [], 1024 * D * QC, 14, (hidden, wdown))

    hidden_r = hid(rem_n, rem2_n)
    hidden_o = hid(own_n, own2_n)
    part, part2 = down(hidden_r)
    s_rem = plus(part, other_core(part2))
    part, part2 = down(hidden_o)
    return plus(mid_own, part, other_core(part2), to_owner(s_rem))


def solution(mesh):
    split = Mesh(
        mesh.devices.reshape(mesh.shape["rep"], 2, 4, 4, mesh.shape["tp"]),
        ("rep", "fs_0", "fs_1", "fs_2", "tp"),
    )
    placed = (
        P(REP_FS_TP, None),
        P(),
        P(FS, "tp"),
        P(FS, "tp"),
        P(),
        P(),
        P(),
        P(),
        P("tp", FS),
        P(),
        P(FS, "tp"),
        P(FS, "tp"),
        P(),
        P("tp", FS),
    )

    return jax.shard_map(on_device, mesh=split, in_specs=placed, out_specs=P(REP_FS_TP, None), check_vma=False)
```

```python
import functools

import jax
import jax.numpy as jnp
from jax import lax
from jax.experimental import pallas as pl
from jax.experimental.pallas import tpu as pltpu
from jax.sharding import Mesh
from jax.sharding import PartitionSpec as P


D = 2048
HEAD = 64
GROUP = 2048
BLOCK = 128
SEGMENT = 64
SEQ = 256
QM = 512
QC = 768
QSTEP = 640
UNITS = 1408
FS = ("fs_0", "fs_1", "fs_2")
REP_FS_TP = ("rep", "fs_0", "fs_1", "fs_2", "tp")
Z = ("rep", "fs_0")
ZT = ("rep", "fs_0", "tp")
YXT = ("fs_1", "fs_2", "tp")
F32 = jnp.float32
BF16 = jnp.bfloat16


def ring(value, axis, by):
    return lax.ppermute(value, axis, [(i, (i + by) % 4) for i in range(4)])


def other_core(value):
    return lax.ppermute(value, "tp", [(0, 1), (1, 0)])


def to_partner(value):
    pairs = []
    for z in range(4):
        pairs.append((2 * z, 2 * ((z - 1) % 4)))
        pairs.append((2 * z + 1, 2 * ((z + 1) % 4) + 1))
    return lax.ppermute(value, ZT, pairs)


def to_owner(value):
    pairs = []
    for z in range(4):
        pairs.append((2 * z, 2 * ((z + 1) % 4)))
        pairs.append((2 * z + 1, 2 * ((z - 1) % 4) + 1))
    return lax.ppermute(value, ZT, pairs)


def along(value, first, by):
    pairs = []
    for y in range(4):
        for x in range(4):
            for t in range(2):
                on_x = (t == 0) == first
                to_x = (x + by) % 4 if on_x else x
                to_y = y if on_x else (y + by) % 4
                pairs.append((y * 8 + x * 2 + t, to_y * 8 + to_x * 2 + t))
    return lax.ppermute(value, YXT, pairs)


def plane_first(piece, route):
    back = along(piece, True, 1)
    ahead = along(piece, True, -1)
    return (piece, ahead, furthest(piece, ahead, back, True, route), back)


def furthest(piece, ahead, back, first, route):
    if route == 0:
        return along(piece, first, 2)
    return along(back, first, 1) if route > 0 else along(ahead, first, -1)


def join_kernel(widths, *refs):
    pieces, outs, sems = refs[:8], refs[8:-1], refs[-1]
    copies = []
    column = 0
    for k, width in enumerate(widths):
        for n, piece in enumerate(pieces):
            copies.append(
                pltpu.make_async_copy(
                    piece.at[:, pl.ds(column, width)], outs[k].at[pl.ds(n * 64, 64), :], sems.at[k * 8 + n]
                )
            )
        column += width
    for c in copies:
        c.start()
    for c in copies:
        c.wait()


def joined(pieces, widths):
    return pl.pallas_call(
        functools.partial(join_kernel, widths),
        out_shape=[jax.ShapeDtypeStruct((512, w), BF16) for w in widths],
        in_specs=[AN] * 8,
        out_specs=[VM] * len(widths),
        scratch_shapes=[pltpu.SemaphoreType.DMA((8 * len(widths),))],
        cost_estimate=pl.CostEstimate(flops=1 << 20, bytes_accessed=4 << 20, transcendentals=0),
        compiler_params=pltpu.CompilerParams(vmem_limit_bytes=6 << 20),
    )(*pieces)


def plane_second(line, route):
    back = along(line, False, 1)
    ahead = along(line, False, -1)
    if route == 2:
        far = (along(back[:256], False, 1), along(ahead[256:], False, -1))
    else:
        far = (furthest(line, ahead, back, False, route),)
    return (line, ahead, *far, back)


PLACES = [(s, f * 128 + h * 64, f, s, h) for s in range(4) for f in range(4) for h in range(2)]


def place_weight(refs, held):
    x = lax.axis_index("fs_2")
    y = lax.axis_index("fs_1")
    a = lax.axis_index("fs_0")
    t = lax.axis_index("tp")
    for which, row, first, second, half in PLACES:
        dx = first + t * (second - first)
        dy = second + t * (first - second)
        block = lax.rem(a + half, 2) * 16 + lax.rem(y + dy, 4) * 4 + lax.rem(x + dx, 4)
        if len(refs) == 5 and (which == 3 or which == 2 and row >= 256):
            which, row = which + 1, row % 256 if which == 2 else row
        held[pl.ds(pl.multiple_of(block * 64, 64), 64), :] = refs[which][row : row + 64, :]


def rms_normed(value, gain):
    wide = value.astype(F32)
    scale = lax.rsqrt(jnp.mean(wide * wide, axis=-1, keepdims=True) + 1e-06)
    return (wide * scale * gain).astype(BF16)


def norm_kernel(rows_in, gain, out):
    @pl.loop(0, SEQ // 32)
    def _(k):
        rows = pl.ds(pl.multiple_of(k * 32, 32), 32)
        out[rows, :] = rms_normed(rows_in[rows, :], gain[...])


def as_row(column):
    return jnp.broadcast_to(column, (BLOCK, BLOCK)).T[0:1, :]


def as_column(row):
    return jnp.broadcast_to(row, (BLOCK, BLOCK)).T


def spatial_kernel(own, own2, rem, rem2, *rest):
    pieces, (act_v, sums), (held,) = rest[:4], rest[4:6], rest[6:]
    t = lax.axis_index("tp")
    place_weight(pieces, held)
    for s, ref in enumerate((own, own2, rem, rem2)):
        v = jnp.dot(ref[...], held[...], preferred_element_type=F32)
        v = jax.nn.gelu(v.astype(BF16).astype(F32))
        act_v[s * SEQ : (s + 1) * SEQ, :] = v
        place = 2 * (s // 2) + lax.rem(s + t, 2)
        total = jnp.sum(v, axis=-1, keepdims=True)
        squares = jnp.sum(v * v, axis=-1, keepdims=True)
        for b in range(2):
            part = slice(b * BLOCK, (b + 1) * BLOCK)
            sums[place, b : b + 1, :] = as_row(total[part])
            sums[place, 2 + b : 3 + b, :] = as_row(squares[part])


def gating_kernel(own, own2, rem, rem2, *rest):
    pieces, (act_u,), (held,) = rest[:4], rest[4:5], rest[5:]
    place_weight(pieces, held)
    for s, ref in enumerate((own, own2, rem, rem2)):
        u = jnp.dot(ref[...], held[...], preferred_element_type=F32)
        act_u[s * SEQ : (s + 1) * SEQ, :] = jax.nn.gelu(u.astype(BF16).astype(F32))


def mix_kernel(pair, act_u, act_v, sums, gain, bias, offset, mix_all, *rest):
    pieces, outs, (held, gated, mix, shift) = rest[:4], rest[4:6], rest[6:]
    t = lax.axis_index("tp")
    a = lax.axis_index("fs_0")
    place_weight(pieces, held)
    start = pl.multiple_of(t * 1024 + a * QM, QM)
    gains = gain[:, pl.ds(start, QM)]
    biases = bias[:, pl.ds(start, QM)]
    lane = lax.broadcasted_iota(jnp.int32, (BLOCK, 128), 1)
    first_head = pl.multiple_of(t * 16 + a * 8, 8)
    offsets = offset[pl.ds(first_head, 8), :]
    for c in range(QM // 128):
        one, two = as_column(offsets[2 * c : 2 * c + 1]), as_column(offsets[2 * c + 1 : 2 * c + 2])
        shift[:, c * 128 : (c + 1) * 128] = jnp.where(lane < HEAD, one, two)
    allowed = lane // SEGMENT <= lax.broadcasted_iota(jnp.int32, (BLOCK, BLOCK), 0) // SEGMENT
    for h in range(8):
        mix[h] = jnp.where(allowed, mix_all[first_head + h].astype(F32), 0.0).astype(BF16)

    @pl.loop(0, 2)
    def _(s):
        place = 2 * pair + lax.rem(s + t, 2)
        for b in range(2):
            here = s * SEQ + b * BLOCK
            rows = pl.ds(pl.multiple_of(2 * pair * SEQ + here, BLOCK), BLOCK)
            to = pl.ds(pl.multiple_of(here, BLOCK), BLOCK)
            mean = as_column(sums[place, b : b + 1, :]) / GROUP
            var = as_column(sums[place, 2 + b : 3 + b, :]) / GROUP - mean * mean
            scale = lax.rsqrt(var + 1e-05)
            for c in range(QM // 128):
                lanes = slice(c * 128, (c + 1) * 128)
                v = (act_v[rows, lanes] - mean) * scale * gains[:, lanes] + biases[:, lanes]
                v = v.astype(BF16)
                one = jnp.dot(mix[2 * c], v, preferred_element_type=F32)
                two = jnp.dot(mix[2 * c + 1], v, preferred_element_type=F32)
                mixed = jnp.where(lane < HEAD, one, two) + shift[:, lanes]
                gated[to, lanes] = (act_u[rows, lanes] * mixed).astype(BF16)

    for s in (1, 0):
        out = lax.dot_general(
            gated[s * SEQ : (s + 1) * SEQ, :], held[...], (((1,), (1,)), ((), ())), preferred_element_type=F32
        )
        outs[s][...] = out.astype(BF16)


def assemble_kernel(sizes, *refs):
    begin = 0
    for k, size in enumerate(sizes):
        place_weight(refs[begin : begin + size], refs[sum(sizes) + k])
        begin += size


def hidden_kernel(first, second, wgate, wup, taps_all, hidden):
    a = lax.axis_index("fs_0")
    t = lax.axis_index("tp")
    taps = taps_all[:, pl.ds(pl.multiple_of(t * UNITS + a * QSTEP, 128), QC)]
    for s, ref in enumerate((first, second)):
        gate = jnp.dot(ref[...], wgate[...], preferred_element_type=F32).astype(BF16).astype(F32)
        up = jnp.dot(ref[...], wup[...], preferred_element_type=F32).astype(BF16).astype(F32)
        row = lax.broadcasted_iota(jnp.int32, gate.shape, 0)
        conv = taps[2:3, :] * gate
        for lag in (1, 2):
            conv = conv + taps[2 - lag : 3 - lag, :] * jnp.where(row >= lag, pltpu.roll(gate, lag, 0), 0.0)
        product = jax.nn.silu(conv) * up
        lane = lax.broadcasted_iota(jnp.int32, gate.shape, 1)
        hidden[s] = jnp.where(lane >= 128 * a, product, 0.0).astype(BF16)


def down_kernel(hidden, wdown, out_first, out_second):
    for s, out_ref in ((1, out_second), (0, out_first)):
        out = lax.dot_general(hidden[s], wdown[...], (((1,), (1,)), ((), ())), preferred_element_type=F32)
        out_ref[...] = out.astype(BF16)


VM = pl.BlockSpec(memory_space=pltpu.VMEM)
AN = pl.BlockSpec(memory_space=pltpu.HBM)


def call(kernel, out_shape, scratch, flops, limit, args):
    return pl.pallas_call(
        kernel,
        out_shape=out_shape,
        in_specs=[VM] * len(args),
        out_specs=jax.tree.map(lambda _: VM, out_shape),
        scratch_shapes=scratch,
        cost_estimate=pl.CostEstimate(flops=int(flops), bytes_accessed=8 << 20, transcendentals=0),
        compiler_params=pltpu.CompilerParams(vmem_limit_bytes=limit << 20),
    )(*args)


def plus_kernel(n, gained, *refs):
    @pl.loop(0, SEQ // 32)
    def _(k):
        rows = pl.ds(pl.multiple_of(k * 32, 32), 32)
        total = refs[0][rows, :].astype(F32)
        for ref in refs[1:n]:
            total = total + ref[rows, :].astype(F32)
        total = total.astype(BF16)
        if gained:
            refs[n + 1][rows, :] = total
            refs[n + 2][rows, :] = rms_normed(total, refs[n][...])
        else:
            refs[n][rows, :] = total


def plus(*arrays, gain=None):
    one = jax.ShapeDtypeStruct((SEQ, D), BF16)
    args = arrays if gain is None else (*arrays, gain)
    return pl.pallas_call(
        functools.partial(plus_kernel, len(arrays), gain is not None),
        out_shape=one if gain is None else (one, one),
        in_specs=[VM] * len(args),
        out_specs=VM if gain is None else (VM, VM),
        cost_estimate=pl.CostEstimate(flops=1 << 20, bytes_accessed=4 << 20, transcendentals=0),
        compiler_params=pltpu.CompilerParams(vmem_limit_bytes=10 << 20),
    )(*args)


def normed(rows, gain):
    return pl.pallas_call(
        norm_kernel,
        out_shape=jax.ShapeDtypeStruct((SEQ, D), BF16),
        in_specs=[VM, VM],
        out_specs=VM,
        cost_estimate=pl.CostEstimate(flops=1 << 20, bytes_accessed=2 << 20, transcendentals=0),
        compiler_params=pltpu.CompilerParams(vmem_limit_bytes=6 << 20),
    )(rows, gain)


def arr(shape, dtype):
    return jax.ShapeDtypeStruct(shape, dtype)


def on_device(
    residual,
    mixer_gain,
    gating_proj,
    spatial_proj,
    spatial_gain,
    spatial_bias,
    spatial_mix,
    spatial_offset,
    mixer_out,
    channel_gain,
    gate_proj,
    up_proj,
    conv_taps,
    down_proj,
):
    a = lax.axis_index("fs_0")

    def window(arrays, which, step, width):
        return jnp.concatenate(
            [lax.dynamic_slice_in_dim(w, which * step, width, 1) for w in arrays], axis=1
        )

    mixer_arrays = (spatial_proj, gating_proj, mixer_out.T)
    channel_arrays = (gate_proj, up_proj, down_proj.T)

    def first_phase(arrays, step, width, routes):
        give = window(arrays, 1 - a, step, width)
        mine = window(arrays, a, step, width)
        theirs = to_owner(give)
        firsts = zip(plane_first(mine, routes[0]), plane_first(theirs, routes[1]))
        return [piece for both in firsts for piece in both]

    own = residual
    rem = to_partner(own)
    own_n = normed(own, mixer_gain[None])
    own2_n = other_core(own_n)
    rem_n = normed(rem, mixer_gain[None])
    rem2_n = other_core(rem_n)
    m_first = first_phase(mixer_arrays, QM, QM, (0, 0))
    s_line, u_line, o_line = joined(m_first, (QM,) * 3)
    s_pieces = plane_second(s_line, 1)
    u_pieces = plane_second(u_line, -1)
    o_pieces = plane_second(o_line, 0)
    c_first = first_phase(channel_arrays, QSTEP, QC, (1, -1))
    g_line, h_line, d_line = joined(c_first, (QC,) * 3)
    g_pieces = plane_second(g_line, 1)
    h_pieces = plane_second(h_line, -1)
    d_pieces = plane_second(d_line, 2)
    seqs = (own_n, own2_n, rem_n, rem2_n)

    act_v, sums = call(
        spatial_kernel,
        (arr((4 * SEQ, QM), F32), arr((4, 4, 128), F32)),
        [pltpu.VMEM((D, QM), BF16)],
        2 * 1024 * D * QM,
        14,
        (*seqs, *s_pieces),
    )
    sums = sums + other_core(sums)
    from_below = ring(sums[1:3], Z, 1)
    from_above = ring(jnp.stack([sums[0], sums[3]]), Z, -1)
    sums = sums + jnp.stack([from_below[1], from_above[1], from_above[0], from_below[0]])
    (act_u,) = call(
        gating_kernel,
        (arr((4 * SEQ, QM), F32),),
        [pltpu.VMEM((D, QM), BF16)],
        2 * 1024 * D * QM,
        14,
        (*seqs, *u_pieces),
    )
    pair = (arr((SEQ, D), BF16),) * 2

    def mixed(k):
        return call(
            functools.partial(mix_kernel, k),
            pair,
            [pltpu.VMEM((D, QM), BF16), pltpu.VMEM((2 * SEQ, QM), BF16), pltpu.VMEM((8, 128, 128), BF16)]
            + [pltpu.VMEM((128, QM), F32)],
            1024 * D * QM,
            16,
            (act_u, act_v, sums, spatial_gain[None], spatial_bias[None], spatial_offset, spatial_mix, *o_pieces),
        )

    part, part2 = mixed(0)
    s_own = plus(part, other_core(part2))
    part, part2 = mixed(1)
    s_rem = plus(part, other_core(part2))
    _, rem_n = plus(rem, s_rem, to_partner(s_own), gain=channel_gain[None])
    mid_own, own_n = plus(own, s_own, to_owner(s_rem), gain=channel_gain[None])
    rem2_n = other_core(rem_n)
    own2_n = other_core(own_n)

    def assembled(*groups):
        flat = [p for g in groups for p in g]
        return pl.pallas_call(
            functools.partial(assemble_kernel, [len(g) for g in groups]),
            out_shape=[arr((D, QC), BF16)] * len(groups),
            in_specs=[VM] * len(flat),
            out_specs=[VM] * len(groups),
            cost_estimate=pl.CostEstimate(flops=1 << 20, bytes_accessed=8 << 20, transcendentals=0),
            compiler_params=pltpu.CompilerParams(vmem_limit_bytes=16 << 20),
        )(*flat)

    wgate, wup = assembled(g_pieces, h_pieces)
    (wdown,) = assembled(d_pieces)

    def hid(first, second):
        (out,) = call(
            hidden_kernel, (arr((2, SEQ, QC), BF16),), [], 2 * 1024 * D * QC, 20, (first, second, wgate, wup, conv_taps)
        )
        return out

    def down(hidden):
        return call(down_kernel, pair, [], 1024 * D * QC, 14, (hidden, wdown))

    hidden_r = hid(rem_n, rem2_n)
    hidden_o = hid(own_n, own2_n)
    part, part2 = down(hidden_r)
    s_rem = plus(part, other_core(part2))
    part, part2 = down(hidden_o)
    return plus(mid_own, part, other_core(part2), to_owner(s_rem))


def solution(mesh):
    split = Mesh(
        mesh.devices.reshape(mesh.shape["rep"], 2, 4, 4, mesh.shape["tp"]),
        ("rep", "fs_0", "fs_1", "fs_2", "tp"),
    )
    placed = (
        P(REP_FS_TP, None),
        P(),
        P(FS, "tp"),
        P(FS, "tp"),
        P(),
        P(),
        P(),
        P(),
        P("tp", FS),
        P(),
        P(FS, "tp"),
        P(FS, "tp"),
        P(),
        P("tp", FS),
    )

    return jax.shard_map(on_device, mesh=split, in_specs=placed, out_specs=P(REP_FS_TP, None), check_vma=False)
```
